32 devices in a mesh: kv: 8 (over z, y), tp: 4 (over x, core).
Axes of the slice: x: 2, y: 2, z: 4, core: 2. Of those that a mesh axis runs over, the one named last changes fastest.
Arguments:
- tokens: bfloat16 [1024, 4096], P(None, 'kv'), may hold values from -6 to 6
- norm_gain: float32 [4096], replicated, may hold values from 0.1 to 1.9
- query_weight: bfloat16 [4096, 2048], P('kv', 'tp'), may hold values from -0.09375 to 0.09375
- key_weight: bfloat16 [4096, 2048], P('kv', 'tp'), may hold values from -0.09375 to 0.09375
- value_weight: bfloat16 [4096, 4096], P('kv', 'tp'), may hold values from -0.09375 to 0.09375
- outgate_weight: bfloat16 [4096, 4096], P('kv', 'tp'), may hold values from -0.09375 to 0.09375
- gate_weight: bfloat16 [4096, 32], P('kv'), may hold values from -0.09375 to 0.09375
- forget_bias: float32 [16], replicated, may hold values from -1 to 5
- head_gain: float32 [4096], P('tp'), may hold values from 0.1 to 1.9
- output_weight: bfloat16 [4096, 4096], P('tp', 'kv'), may hold values from -0.09375 to 0.09375
- state_matrix: float32 [256, 16, 128, 256], P('kv', 'tp'), may hold values from -6 to 6
- state_normal: float32 [256, 16, 128], P('kv', 'tp'), may hold values from -6 to 6
- state_stable: float32 [256, 16], P('kv', 'tp'), may hold values from -3 to 3
- prior_keys: bfloat16 [256, 4, 2048], P('kv', None, 'tp'), may hold values from -0.59765625 to 0.59765625
- prior_values: bfloat16 [256, 4, 4096], P('kv', None, 'tp'), may hold values from -6 to 6
- prior_ingate: float32 [256, 4, 16], P('kv', None, 'tp'), may hold values from -4 to 4
- prior_forget: float32 [256, 4, 16], P('kv', None, 'tp'), may hold values from -2 to -0.02
- accepted: int32 [256], P('kv'), may hold values from 0 to 4
- parents: int32 [256, 4], P('kv'), may hold values from -1 to 2, as said below
Outputs:
- layer_out: bfloat16 [1024, 4096], P('tp', 'kv')
- new_matrix: float32 [256, 16, 128, 256], P('kv', 'tp')
- new_normal: float32 [256, 16, 128], P('kv', 'tp')
- new_stable: float32 [256, 16], P('kv', 'tp')
The draws below stay inside these ranges and needn't reach their ends.
Inputs may be any that keep to these rules, and one draw needn't show every extreme that they name: parents of proposal t lie in -1 to t - 1; the first proposal's parent is -1; in some sequence each proposal's parent is the one before it.
All inputs are finite; a program needn't handle non-finite values.
Results may differ from the reference program's by a relative error of at most 0.0089.
Values may be sent and summed in bfloat16 or wider, within the bound.
No kernel may reach another device: no remote copies, remote signals or barrier semaphores. Data moves between devices by JAX's collectives and lax.ppermute only.
A program may use at most 128 MiB of HBM per device.

```python
import jax
import jax.numpy as jnp
from jax import lax

D = 4096
HEADS = 16
DQK = 128
DV = 256
PROP = 4
SEQS = 256
TOKENS = 1024


def draw_parents(key, part):
    random_ints = jax.random.randint(key, (SEQS, PROP), 0, 1 << 20)
    position = jnp.arange(PROP, dtype=jnp.int32)[None, :]
    chosen = random_ints % jnp.maximum(position, 1)
    leading = jnp.arange(SEQS, dtype=jnp.int32)[:, None] == 0
    chosen = jnp.where(leading, position - 1, chosen)
    return jnp.where(position == 0, -1, chosen).astype(jnp.int32)


def set_ends(entries, rng, least, top_value):
    dims = entries.shape
    place = [jax.random.randint(jax.random.fold_in(rng, axis), (), 0, dims[axis]) for axis in range(len(dims))]
    entries = entries.at[tuple(place)].set(least)
    longest = dims.index(max(dims))
    place[longest] = (place[longest] + 1) % dims[longest]
    return entries.at[tuple(place)].set(top_value)


def block_scale(rng, shape, shards, least, largest):
    def one(axis_at, parts):
        steps = jax.random.uniform(jax.random.fold_in(jax.random.fold_in(rng, 6), axis_at), (parts,), jnp.float32, least / len(shards), largest / len(shards))
        return jnp.repeat(jnp.exp(steps), shape[axis_at] // parts).reshape((-1,) + (1,) * (len(shape) - axis_at - 1))

    factor_of = one(*shards[0])
    for cut in shards[1:]:
        factor_of = factor_of * one(*cut)
    return factor_of


def centred(rng, dims, scale, most, shards=(), kind=jnp.bfloat16):
    loudness = block_scale(rng, dims, shards, -0.22, 0.18) if shards else 1.0
    array = jax.random.normal(rng, dims, jnp.float32) * scale * loudness
    return jnp.minimum(jnp.maximum(array, -most), most).astype(kind)


def setup_inputs(seed: int = 0) -> dict:
    keys = jax.random.split(jax.random.key(seed), 20)
    return {
        "tokens": centred(keys[0], (TOKENS, D), 1.0, 6.0, ((1, 8),)),
        "norm_gain": jnp.clip(1.0 + 0.18 * jax.random.normal(keys[1], (D,), jnp.float32), 0.1, 1.9),
        "query_weight": centred(keys[2], (D, HEADS * DQK), D ** -0.5, 0.09375, ((0, 8), (1, 4))),
        "key_weight": centred(keys[3], (D, HEADS * DQK), D ** -0.5, 0.09375, ((0, 8), (1, 4))),
        "value_weight": centred(keys[4], (D, HEADS * DV), D ** -0.5, 0.09375, ((0, 8), (1, 4))),
        "outgate_weight": centred(keys[5], (D, HEADS * DV), D ** -0.5, 0.09375, ((0, 8), (1, 4))),
        "gate_weight": centred(keys[6], (D, 2 * HEADS), D ** -0.5, 0.09375, ((0, 8),)),
        "forget_bias": jnp.clip(jax.random.uniform(keys[7], (HEADS,), jnp.float32, -1.0, 5.0), -1.0, 5.0),
        "head_gain": jnp.clip(1.0 + 0.18 * jax.random.normal(keys[8], (HEADS * DV,), jnp.float32), 0.1, 1.9),
        "output_weight": centred(keys[9], (HEADS * DV, D), (HEADS * DV) ** -0.5, 0.09375, ((0, 4), (1, 8))),
        "state_matrix": centred(keys[10], (SEQS, HEADS, DQK, DV), 1.0, 6.0, ((0, 8), (1, 4)), jnp.float32),
        "state_normal": centred(keys[11], (SEQS, HEADS, DQK), 1.0, 6.0, ((0, 8), (1, 4)), jnp.float32),
        "state_stable": centred(keys[12], (SEQS, HEADS), 1.0, 3.0, ((0, 8), (1, 4)), jnp.float32),
        "prior_keys": centred(keys[13], (SEQS, PROP, HEADS * DQK), 0.09, 0.59765625, ((0, 8), (2, 4))),
        "prior_values": centred(keys[14], (SEQS, PROP, HEADS * DV), 1.0, 6.0, ((0, 8), (2, 4))),
        "prior_ingate": centred(keys[15], (SEQS, PROP, HEADS), 1.0, 4.0, ((0, 8), (2, 4)), jnp.float32),
        "prior_forget": jnp.clip(-2.0 + 1.98 * jax.random.uniform(keys[16], (SEQS, PROP, HEADS), jnp.float32) ** block_scale(keys[16], (SEQS, PROP, HEADS), ((0, 8), (2, 4)), -0.2, 0.2), -2.0, -0.02),
        "accepted": set_ends(jax.random.randint(keys[17], (SEQS,), 0, PROP + 1), jax.random.fold_in(keys[17], 1), 0, PROP).astype(jnp.int32),
        "parents": draw_parents(jax.random.fold_in(keys[19], 71), 0),
    }


def ancestry(parents):
    count = parents.shape[1]
    index = jnp.arange(count, dtype=jnp.int32)
    current = jnp.broadcast_to(index[None, :], parents.shape).astype(jnp.int32)
    table = jnp.broadcast_to((index[:, None] == index[None, :]).astype(jnp.float32), (parents.shape[0], count, count))
    for repeat in range(count - 1):
        looked = jnp.take_along_axis(parents, jnp.maximum(current, 0), axis=1)
        current = jnp.where(current >= 0, looked, -1).astype(jnp.int32)
        table = table + (current[:, :, None] == index[None, None, :]).astype(jnp.float32)
    return table

def commit(matrix, normal, stable, prior_k, prior_v, prior_i, prior_f, accepted):
    count = prior_k.shape[1]
    live = (jnp.arange(count, dtype=jnp.int32)[None, :] < accepted[:, None])[:, :, None]
    forget_live = jnp.where(live, prior_f, 0.0)
    cumul = jnp.cumsum(forget_live, axis=1)
    total = cumul[:, -1]
    weight_log = jnp.where(live, total[:, None, :] - cumul + prior_i, -jnp.inf)
    new_stable = jnp.maximum(total + stable, lax.optimization_barrier(jnp.max(weight_log, axis=1)))
    weights = jnp.exp(weight_log - new_stable[:, None, :])
    decay = jnp.exp(total + stable - new_stable)
    hp = lax.Precision.HIGHEST
    new_matrix = decay[:, :, None, None] * matrix + jnp.einsum('sph,sphd,sphv->shdv', weights, prior_k, prior_v, precision=hp)
    new_normal = decay[:, :, None] * normal + jnp.einsum('sph,sphd->shd', weights, prior_k, precision=hp)
    return (new_matrix, new_normal, new_stable)

def tree_read(query, key_rows, value_rows, ingate, logforget, table, matrix, normal, stable):
    hp = lax.Precision.HIGHEST
    path_sum = jnp.einsum('sta,sah->sth', table, logforget, precision=hp)
    dlog = path_sum[:, :, None, :] - path_sum[:, None, :, :] + ingate[:, None, :, :]
    dlog = jnp.where(table[:, :, :, None] > 0.5, dlog, -jnp.inf)
    carried = path_sum + stable[:, None, :]
    top = jnp.maximum(carried, lax.optimization_barrier(jnp.max(dlog, axis=2)))
    scores = jnp.einsum('sthd,sahd->stah', query, key_rows, precision=hp) * jnp.exp(dlog - top[:, :, None, :])
    factor = jnp.exp(carried - top)
    numer = jnp.einsum('stah,sahv->sthv', scores, value_rows, precision=hp) + factor[..., None] * jnp.einsum('sthd,shdv->sthv', query, matrix, precision=hp)
    denom = lax.optimization_barrier(jnp.sum(scores, axis=2)) + factor * jnp.einsum('sthd,shd->sth', query, normal, precision=hp)
    return numer / jnp.maximum(jnp.abs(denom), jnp.exp(-top))[..., None]

def reference(tokens, norm_gain, query_weight, key_weight, value_weight, outgate_weight, gate_weight, forget_bias, head_gain, output_weight, state_matrix, state_normal, state_stable, prior_keys, prior_values, prior_ingate, prior_forget, accepted, parents):
    f32 = jnp.float32
    xfloat = tokens.astype(f32)
    scale = lax.rsqrt(lax.optimization_barrier(jnp.sum(xfloat * xfloat, axis=-1, keepdims=True)) / D + 1e-06)
    normed = (xfloat * norm_gain).astype(jnp.bfloat16)
    query = scale * jnp.dot(normed, query_weight, preferred_element_type=f32)
    key_rows = scale * jnp.dot(normed, key_weight, preferred_element_type=f32) / jnp.sqrt(jnp.float32(DQK))
    value_rows = scale * jnp.dot(normed, value_weight, preferred_element_type=f32)
    outgate = scale * jnp.dot(normed, outgate_weight, preferred_element_type=f32)
    gates = scale * jnp.dot(normed, gate_weight, preferred_element_type=f32)
    ingate = gates[:, :HEADS].reshape(SEQS, PROP, HEADS)
    logforget = jax.nn.log_sigmoid(gates[:, HEADS:] + forget_bias).reshape(SEQS, PROP, HEADS)
    new_matrix, new_normal, new_stable = commit(state_matrix, state_normal, state_stable, prior_keys.astype(f32).reshape(SEQS, PROP, HEADS, DQK), prior_values.astype(f32).reshape(SEQS, PROP, HEADS, DV), prior_ingate, prior_forget, accepted)
    table = ancestry(parents)
    read = tree_read(query.reshape(SEQS, PROP, HEADS, DQK), key_rows.reshape(SEQS, PROP, HEADS, DQK), value_rows.reshape(SEQS, PROP, HEADS, DV), ingate, logforget, table, new_matrix, new_normal, new_stable)
    normer = lax.rsqrt(lax.optimization_barrier(jnp.mean(read * read, axis=-1, keepdims=True)) + 1e-06)
    hidden = read * normer * head_gain.reshape(HEADS, DV) * jax.nn.sigmoid(outgate.reshape(SEQS, PROP, HEADS, DV))
    hidden = hidden.reshape(TOKENS, HEADS * DV).astype(jnp.bfloat16)
    layer_out = jnp.dot(hidden, output_weight, preferred_element_type=f32).astype(jnp.bfloat16)
    return (layer_out, new_matrix, new_normal, new_stable)
```

```python
import functools

import jax
import jax.numpy as jnp
from jax import lax
from jax.experimental import pallas as pl
from jax.experimental.pallas import tpu as pltpu
from jax.sharding import PartitionSpec as P

D = 4096
HEADS = 16
DQK = 128
DV = 256
PROP = 4
CHUNKS = 4


F32 = jnp.float32
BF16 = jnp.bfloat16
HIGHEST = lax.Precision.HIGHEST


def ancestry(parents):
    count = parents.shape[1]
    index = jnp.arange(count, dtype=jnp.int32)[None, :]
    rows = []
    for t in range(count):
        row = jnp.broadcast_to((index == t).astype(F32), parents.shape)
        for p in range(t):
            row = row + (parents[:, t : t + 1] == p).astype(F32) * rows[p]
        rows.append(row)
    return jnp.stack(rows, axis=1)


def commit(matrix, normal, stable, prior_k, prior_v, prior_i, prior_f, accepted):
    count = prior_k.shape[1]
    live = (jnp.arange(count, dtype=jnp.int32)[None, :] < accepted[:, None])[:, :, None]
    forget_live = jnp.where(live, prior_f, 0.0)
    parts = [forget_live[:, 0]]
    for s in range(1, count):
        parts.append(parts[-1] + forget_live[:, s])
    cumul = jnp.stack(parts, axis=1)
    total = parts[-1]
    weight_log = jnp.where(live, total[:, None, :] - cumul + prior_i, -jnp.inf)
    new_stable = jnp.maximum(total + stable, jnp.max(weight_log, axis=1))
    weights = jnp.exp(weight_log - new_stable[:, None, :])
    decay = jnp.exp(total + stable - new_stable)
    new_matrix = decay[:, :, None, None] * matrix + jnp.einsum(
        "sph,sphd,sphv->shdv", weights, prior_k, prior_v, precision=HIGHEST
    )
    new_normal = decay[:, :, None] * normal + jnp.einsum(
        "sph,sphd->shd", weights, prior_k, precision=HIGHEST
    )
    return (new_matrix, new_normal, new_stable)


def project_body(x_ref, wq_ref, wk_ref, wv_ref, wg_ref, out_ref):
    x = x_ref[...]
    at = 0
    for w_ref in (wq_ref, wk_ref, wv_ref, wg_ref):
        width = w_ref.shape[1]
        out_ref[:, at : at + width] = jnp.dot(
            x, w_ref[...], preferred_element_type=F32
        ).astype(out_ref.dtype)
        at += width


def weight_specs(width_local):
    return [
        pl.BlockSpec((width_local, DQK), lambda h: (0, h)),
        pl.BlockSpec((width_local, DQK), lambda h: (0, h)),
        pl.BlockSpec((width_local, DV), lambda h: (0, h)),
        pl.BlockSpec((width_local, DV), lambda h: (0, h)),
    ]


HEAD_COLS = 2 * DQK + 2 * DV


def project(rows, weights, head_local):
    count, width = rows.shape
    return pl.pallas_call(
        project_body,
        grid=(head_local,),
        in_specs=[pl.BlockSpec((count, width), lambda h: (0, 0))] + weight_specs(width),
        out_specs=pl.BlockSpec((count, HEAD_COLS), lambda h: (0, h)),
        out_shape=jax.ShapeDtypeStruct((count, head_local * HEAD_COLS), BF16),
        cost_estimate=pl.CostEstimate(
            flops=2 * count * width * head_local * HEAD_COLS,
            bytes_accessed=2 * (count + width) * head_local * HEAD_COLS,
            transcendentals=0,
        ),
        name="project_other",
    )(rows, *weights)


def project_add_body(x_ref, other_ref, wq_ref, wk_ref, wv_ref, wg_ref, own_ref, *send_refs):
    x = x_ref[...]
    block = own_ref.shape[0]
    at = 0
    for w_ref in (wq_ref, wk_ref, wv_ref, wg_ref):
        width = w_ref.shape[1]
        cols = slice(at, at + width)
        total = jnp.dot(x, w_ref[...], preferred_element_type=F32) + other_ref[:, cols].astype(F32)
        own_ref[:, cols] = total[:block]
        for j, send_ref in enumerate(send_refs):
            send_ref[:, cols] = total[(j + 1) * block : (j + 2) * block].astype(BF16)
        at += width


def project_add(rows, other, weights, head_local, half):
    count, width = rows.shape
    block = count // half
    spec = pl.BlockSpec((block, HEAD_COLS), lambda h: (0, h))
    cols = head_local * HEAD_COLS
    return pl.pallas_call(
        project_add_body,
        grid=(head_local,),
        in_specs=[
            pl.BlockSpec((count, width), lambda h: (0, 0)),
            pl.BlockSpec((count, HEAD_COLS), lambda h: (0, h)),
        ]
        + weight_specs(width),
        out_specs=[spec] * half,
        out_shape=[jax.ShapeDtypeStruct((block, cols), F32)]
        + [jax.ShapeDtypeStruct((block, cols), BF16)] * (half - 1),
        cost_estimate=pl.CostEstimate(
            flops=2 * count * width * cols,
            bytes_accessed=2 * (2 * count + width) * cols,
            transcendentals=0,
        ),
        name="project_own",
    )(rows, other, *weights)


def read_body(parts, head_local, own_ref, *refs):
    got = refs[:parts]
    mat_ref, norm_ref, wmat_ref, cols_ref, gain_ref, hid_ref = refs[parts:]
    rows = own_ref.shape[0]
    seqs = mat_ref.shape[0]
    prop = rows // seqs
    row_seq = lax.broadcasted_iota(jnp.int32, (rows, seqs), 0) // prop
    pick = (row_seq == lax.broadcasted_iota(jnp.int32, (rows, seqs), 1)).astype(F32)
    lane_seq = lax.broadcasted_iota(jnp.int32, (rows, seqs * DQK), 1) // DQK
    big_seq = lax.broadcasted_iota(jnp.int32, (rows, seqs * DQK), 0) // prop
    big_pick = lane_seq == big_seq
    nt = (((1,), (1,)), ((), ()))
    for h in range(head_local):
        base = h * HEAD_COLS

        def total(at, width):
            cols = slice(base + at, base + at + width)
            acc = own_ref[:, cols]
            for ref in got:
                acc = acc + ref[:, cols].astype(F32)
            return acc

        scale = cols_ref[h, :, 0:1]
        factor = cols_ref[h, :, 1:2]
        floor = cols_ref[h, :, 2:3]
        query = scale * total(0, DQK)
        key = scale * total(DQK, DQK)
        value = scale * total(2 * DQK, DV)
        gate = scale * total(2 * DQK + DV, DV)
        scores = (
            lax.dot_general(query, key, nt, precision=HIGHEST, preferred_element_type=F32)
            * wmat_ref[h]
        )
        numer = jnp.dot(scores, value, precision=HIGHEST, preferred_element_type=F32)
        spread = jnp.where(big_pick, jnp.concatenate([query] * seqs, axis=1), 0.0).astype(BF16)
        mat = mat_ref[:, h].reshape(seqs * DQK, DV)
        carried = jnp.dot(spread, mat, preferred_element_type=F32)
        qn = lax.dot_general(query, norm_ref[h], nt, precision=HIGHEST, preferred_element_type=F32)
        denom = jnp.sum(scores, axis=1, keepdims=True) + factor * jnp.sum(
            qn * pick, axis=1, keepdims=True
        )
        read = (numer + factor * carried) / jnp.maximum(jnp.abs(denom), floor)
        normer = lax.rsqrt(jnp.mean(read * read, axis=1, keepdims=True) + 1e-06)
        gain = gain_ref[:, h * DV : (h + 1) * DV]
        hid_ref[:, h * DV : (h + 1) * DV] = (
            read * normer * gain * jax.nn.sigmoid(gate)
        ).astype(BF16)


def tree_read(chunk, own, got, mat, norm, wmat, cols, gain, head_local):
    rows = own.shape[0]
    seqs = rows // PROP
    full = lambda shape: pl.BlockSpec(shape, lambda i: (0,) * len(shape))
    return pl.pallas_call(
        functools.partial(read_body, len(got), head_local),
        grid=(1,),
        in_specs=[full(own.shape)]
        + [full(g.shape) for g in got]
        + [
            pl.BlockSpec((seqs,) + mat.shape[1:], lambda i: (chunk, 0, 0, 0)),
            pl.BlockSpec((head_local, seqs, DQK), lambda i: (0, chunk, 0)),
            pl.BlockSpec((None,) + wmat.shape[1:], lambda i: (chunk, 0, 0, 0)),
            pl.BlockSpec((head_local, rows, cols.shape[2]), lambda i: (0, chunk, 0)),
            full(gain.shape),
        ],
        out_specs=full((rows, head_local * DV)),
        out_shape=jax.ShapeDtypeStruct((rows, head_local * DV), BF16),
        cost_estimate=pl.CostEstimate(
            flops=8 * rows * seqs * head_local * DQK * DV,
            bytes_accessed=2 * seqs * head_local * DQK * DV,
            transcendentals=0,
        ),
        name="tree_read",
    )(own, *got, mat, norm, wmat, cols, gain)


def output_body(half, pos_ref, own_ref, *refs):
    got = refs[: half - 1]
    other_ref, w_ref, keep_ref, send_ref = refs[half - 1 :]
    rows = own_ref.shape[0]
    z = pos_ref[0]
    y = pos_ref[1]
    core = pos_ref[2]
    x = pos_ref[3]
    pairs = half // 2
    mine = jnp.concatenate([own_ref[...]] + [ref[...] for ref in got], axis=0)
    weight = w_ref[...]
    outs = (
        jnp.dot(mine, weight, preferred_element_type=F32),
        jnp.dot(other_ref[...], weight, preferred_element_type=F32),
    )
    for j in range(half):
        at = lax.rem(z - j + half, half)
        place = lax.rem(at // 2 - x + pairs, pairs)
        here = lax.rem(at, 2) == core
        for side, out in enumerate(outs):
            row = y if side == 0 else 1 - y
            piece = out[j * rows : (j + 1) * rows]

            @pl.when(here)
            def _():
                keep_ref[place, row] = piece

            @pl.when(jnp.logical_not(here))
            def _():
                send_ref[place, row] = piece


def output_product(pos, own, got, other, weight):
    rows = own.shape[0]
    half = len(got) + 1
    full = lambda shape: pl.BlockSpec(shape, lambda i, *_: (0,) * len(shape))
    shape = (half // 2, 2, rows, weight.shape[1])
    return pl.pallas_call(
        functools.partial(output_body, half),
        grid_spec=pltpu.PrefetchScalarGridSpec(
            num_scalar_prefetch=1,
            grid=(1,),
            in_specs=[full(own.shape)] + [full(g.shape) for g in got] + [full(other.shape), full(weight.shape)],
            out_specs=[full(shape), full(shape)],
        ),
        out_shape=[jax.ShapeDtypeStruct(shape, F32)] * 2,
        cost_estimate=pl.CostEstimate(
            flops=4 * half * rows * weight.shape[0] * weight.shape[1],
            bytes_accessed=2 * weight.shape[0] * weight.shape[1],
            transcendentals=0,
        ),
        name="output_product",
    )(pos, own, *got, other, weight)


def per_device(
    kv_size,
    tp_size,
    tokens,
    norm_gain,
    query_weight,
    key_weight,
    value_weight,
    outgate_weight,
    gate_weight,
    forget_bias,
    head_gain,
    output_weight,
    state_matrix,
    state_normal,
    state_stable,
    prior_keys,
    prior_values,
    prior_ingate,
    prior_forget,
    accepted,
    parents,
):
    head_local = query_weight.shape[1] // DQK
    width_local = tokens.shape[1]
    seq_local = accepted.shape[0]
    row_local = seq_local * PROP
    half = kv_size // 2
    pairs = tp_size // 2
    rows = row_local // CHUNKS
    seqs = rows // PROP
    kv_at = lax.axis_index("kv")
    tp_at = lax.axis_index("tp")
    z, y = kv_at // 2, kv_at % 2
    x, core = tp_at // 2, tp_at % 2
    pos = jnp.stack([z, y, core, x]).astype(jnp.int32)
    flip_y = [(i, i ^ 1) for i in range(kv_size)]
    flip_core = [(i, i ^ 1) for i in range(tp_size)]

    def shift_z(value, by):
        return lax.ppermute(
            value, "kv", [(i, (i // 2 + by) % half * 2 + i % 2) for i in range(kv_size)]
        )

    def shift_x(value, by):
        return lax.ppermute(
            value, "tp", [(i, (i // 2 + by) % pairs * 2 + i % 2) for i in range(tp_size)]
        )

    def arrange(value):
        blocks = value.reshape((half, 2, row_local) + value.shape[1:])
        twice = jnp.concatenate([blocks, blocks], axis=0)
        zero = (0,) * (value.ndim - 1)
        size = (half, 1, row_local) + value.shape[1:]
        own = lax.dynamic_slice(twice, (z, y, 0) + zero, size)
        other = lax.dynamic_slice(twice, (z, 1 - y, 0) + zero, size)
        return own[:, 0], other[:, 0]

    xfloat = tokens.astype(F32)
    own_gain = lax.dynamic_slice_in_dim(norm_gain, kv_at * width_local, width_local, 0)
    normed = (xfloat * own_gain).astype(BF16)
    normed_own, normed_other = arrange(normed)

    def chunked(value):
        split = value.reshape(half, CHUNKS, rows, width_local)
        return split.transpose(1, 0, 2, 3).reshape(CHUNKS, half * rows, width_local)

    normed_own = chunked(normed_own)
    normed_other = chunked(normed_other)
    weights = (query_weight, key_weight, value_weight, outgate_weight)

    gate_cols = lax.dynamic_slice_in_dim(
        gate_weight.reshape(width_local, 2, HEADS), tp_at * head_local, head_local, 2
    ).reshape(width_local, 2 * head_local)
    part_gates = lax.dot_general(
        gate_cols, normed, (((0,), (1,)), ((), ())), preferred_element_type=F32
    )
    part_squares = jnp.sum(xfloat * xfloat, axis=-1)
    small = jnp.concatenate([part_gates, part_squares[None]], axis=0).T
    small_own, small_other = arrange(small)
    small_sum = small_own + lax.ppermute(small_other, "kv", flip_y)
    small_total = small_sum[0]
    for by in range(1, half):
        small_total = small_total + shift_z(small_sum[by], by)
    small_total = small_total.T

    sent = [project(normed_other[c], weights, head_local) for c in range(CHUNKS)]
    across = [lax.ppermute(value, "kv", flip_y) for value in sent]

    new_matrix, new_normal, new_stable = commit(
        state_matrix,
        state_normal,
        state_stable,
        prior_keys.astype(F32).reshape(seq_local, PROP, head_local, DQK),
        prior_values.astype(F32).reshape(seq_local, PROP, head_local, DV),
        prior_ingate,
        prior_forget,
        accepted,
    )
    matrix_low = new_matrix.astype(BF16)
    normal_heads = new_normal.transpose(1, 0, 2)

    scale = lax.rsqrt(small_total[2 * head_local] / D + 1e-06)
    gates = small_total[: 2 * head_local] * scale[None]
    own_bias = lax.dynamic_slice_in_dim(forget_bias, tp_at * head_local, head_local, 0)
    ingate = gates[:head_local].reshape(head_local, CHUNKS, rows)
    logforget = jax.nn.log_sigmoid(gates[head_local:] + own_bias[:, None]).reshape(
        head_local, CHUNKS, rows
    )
    table = ancestry(parents).reshape(CHUNKS, seqs, PROP, PROP)
    same = jnp.eye(seqs, dtype=F32)
    path = (table[:, :, :, None, :] * same[None, :, None, :, None]).reshape(CHUNKS, rows, rows)
    path_sum = jnp.sum(path[None] * logforget[:, :, None, :], axis=3)
    dlog = path_sum[:, :, :, None] - path_sum[:, :, None, :] + ingate[:, :, None, :]
    dlog = jnp.where(path[None] > 0.5, dlog, -jnp.inf)
    stable_rows = jnp.repeat(new_stable.T, PROP, axis=1).reshape(head_local, CHUNKS, rows)
    carried = path_sum + stable_rows
    top = jnp.maximum(carried, jnp.max(dlog, axis=3))
    wmat = (jnp.exp(dlog - top[:, :, :, None]) / jnp.sqrt(F32(DQK))).transpose(1, 0, 2, 3)
    cols = jnp.stack(
        [
            jnp.broadcast_to(scale[None], (head_local, row_local)),
            jnp.exp(carried - top).reshape(head_local, row_local),
            jnp.exp(-top).reshape(head_local, row_local),
        ],
        axis=2,
    )
    gain = head_gain[None, :]

    pieces = []
    for c in range(CHUNKS):
        own, *sends = project_add(normed_own[c], across[c], weights, head_local, half)
        got = [shift_z(value, by + 1) for by, value in enumerate(sends)]
        hidden = tree_read(c, own, got, matrix_low, normal_heads, wmat, cols, gain, head_local)
        near = [shift_z(hidden, by) for by in range(1, half)]
        other = lax.ppermute(jnp.concatenate([hidden] + near, axis=0), "kv", flip_y)
        keep, send = output_product(pos, hidden, near, other, output_weight)
        total = keep + lax.ppermute(send, "tp", flip_core)
        final = total[0]
        for by in range(1, pairs):
            final = final + shift_x(total[by].astype(BF16), by).astype(F32)
        pieces.append(final.astype(BF16))
    layer_out = jnp.stack(pieces, axis=1).reshape(2 * row_local, -1)
    return (layer_out, new_matrix, new_normal, new_stable)


def solution(mesh):
    placed = (
        P(None, "kv"),
        P(),
        P("kv", "tp"),
        P("kv", "tp"),
        P("kv", "tp"),
        P("kv", "tp"),
        P("kv", None),
        P(),
        P("tp"),
        P("tp", "kv"),
        P("kv", "tp", None, None),
        P("kv", "tp", None),
        P("kv", "tp"),
        P("kv", None, "tp"),
        P("kv", None, "tp"),
        P("kv", None, "tp"),
        P("kv", None, "tp"),
        P("kv"),
        P("kv", None),
    )
    kv_size = mesh.shape["kv"]
    tp_size = mesh.shape["tp"]
    assert kv_size == 2 * tp_size
    return jax.shard_map(
        functools.partial(per_device, kv_size, tp_size),
        mesh=mesh,
        in_specs=placed,
        out_specs=(P("tp", "kv"), P("kv", "tp", None, None), P("kv", "tp", None), P("kv", "tp")),
        check_vma=False,
    )
```

```python
import functools

import jax
import jax.numpy as jnp
from jax import lax
from jax.experimental import pallas as pl
from jax.experimental.pallas import tpu as pltpu
from jax.sharding import PartitionSpec as P


D = 4096
HEADS = 16
DQK = 128
DV = 256
PROP = 4
PLAN = ((3, False), (3, False), (2, False))
ORDER = ("g0", "p1", "o0", "m0", "p2", "f0", "m1", "s0", "m2", "f1", "w0", "r0", "f2", "c0", "c1", "r1", "r2")
COMMITS = (2, 2, 2, 2)
OUTPUTS = ((0, 1), (2,))
SPREAD_AFTER = (("c0", "r1"), ("r2", "r2"), ("r2",))
TOKEN = (8, 128)
VMEM_LIMIT = 20 * 1024 * 1024
VMEM_MOST = 48 * 1024 * 1024
VMEM_ALL = 60 * 1024 * 1024


F32 = jnp.float32
BF16 = jnp.bfloat16
HIGHEST = lax.Precision.HIGHEST


def commit(normal, stable, prior_k, prior_i, prior_f, accepted):
    count = prior_k.shape[1]
    live = (jnp.arange(count, dtype=jnp.int32)[None, :] < accepted[:, None])[:, :, None]
    forget_live = jnp.where(live, prior_f, 0.0)
    parts = [forget_live[:, 0]]
    for s in range(1, count):
        parts.append(parts[-1] + forget_live[:, s])
    cumul = jnp.stack(parts, axis=1)
    total = parts[-1]
    weight_log = jnp.where(live, total[:, None, :] - cumul + prior_i, -jnp.inf)
    new_stable = jnp.maximum(total + stable, jnp.max(weight_log, axis=1))
    weights = jnp.exp(weight_log - new_stable[:, None, :])
    decay = jnp.exp(total + stable - new_stable)
    new_normal = decay[:, :, None] * normal + jnp.einsum(
        "sph,sphd->shd", weights, prior_k, precision=HIGHEST
    )
    return (decay, weights, new_normal, new_stable)


def commit_body(mat_ref, left_ref, right_ref, decay_ref, *refs):
    out_ref, token_ref = refs[-2:]
    token_ref[...] = jnp.zeros_like(token_ref)
    seqs, head_local = mat_ref.shape[:2]
    for s in range(seqs):
        for h in range(head_local):
            added = lax.dot_general(
                left_ref[s, :, h * DQK : (h + 1) * DQK],
                right_ref[s, :, h * DV : (h + 1) * DV],
                (((0,), (0,)), ((), ())),
                preferred_element_type=F32,
            )
            out_ref[s, h] = decay_ref[s, :, h : h + 1] * mat_ref[s, h] + added


def commit_factors(prior_k, prior_v, weights):
    key = prior_k.astype(F32) * jnp.repeat(weights, DQK, axis=2)
    high = key.astype(BF16)
    rest = key - high.astype(F32)
    middle = rest.astype(BF16)
    low = (rest - middle.astype(F32)).astype(BF16)
    left = jnp.concatenate([high, middle, low, jnp.zeros_like(low)], axis=1)
    right = jnp.concatenate([prior_v, prior_v, prior_v, jnp.zeros_like(prior_v)], axis=1)
    return left, right


def commit_matrix(first, count, matrix, left, right, decay, before, after):
    head_local = matrix.shape[1]
    step = 4 if count % 4 == 0 and first % 4 == 0 else 1
    start = first // step
    block = pl.BlockSpec((step,) + matrix.shape[1:], lambda s: (start + s, 0, 0, 0))
    rows = lambda array: pl.BlockSpec((step,) + array.shape[1:], lambda s: (start + s, 0, 0))
    anywhere = pl.BlockSpec(memory_space=pl.ANY)
    operands = [matrix, left, right, decay, after]
    specs = [block, rows(left), rows(right), rows(decay), anywhere]
    aliases = {}
    if before is not None:
        aliases = {len(operands): 0}
        operands.append(before)
        specs.append(anywhere)
    return pl.pallas_call(
        commit_body,
        grid=(count // step,),
        in_specs=specs,
        out_specs=[block, full_spec(TOKEN)],
        out_shape=[jax.ShapeDtypeStruct(matrix.shape, F32), jax.ShapeDtypeStruct(TOKEN, F32)],
        input_output_aliases=aliases,
        compiler_params=pltpu.CompilerParams(vmem_limit_bytes=VMEM_ALL),
        cost_estimate=pl.CostEstimate(
            flops=32 * count * head_local * left.shape[1] * DQK * DV,
            bytes_accessed=8 * count * head_local * DQK * DV,
            transcendentals=0,
        ),
        name="commit_matrix",
    )(*operands)


def small_body(head_local, pos_ref, x_ref, gain_ref, gate_ref, _, keep_ref, send_ref):
    kv_at = pos_ref[0]
    count, rows, width = x_ref.shape
    half = count // 2
    nt = (((1,), (1,)), ((), ()))
    index = lax.broadcasted_iota(jnp.int32, (16, 2 * HEADS), 0)
    column = lax.broadcasted_iota(jnp.int32, (16, 2 * HEADS), 1)
    wanted = jnp.where(index < head_local, index, index - head_local + HEADS)
    pick = (index < 2 * head_local) & (column == wanted + pos_ref[1] * head_local)
    last = lax.broadcasted_iota(jnp.int32, (16, rows), 0) == 2 * head_local
    ones = jnp.ones((16, width), BF16)
    for k in range(count):
        x = x_ref[k].astype(F32)
        normed = (x * gain_ref[...]).astype(BF16)
        gates = lax.dot_general(gate_ref[...], normed, nt, preferred_element_type=F32)
        own = jnp.dot(pick.astype(F32), gates, precision=HIGHEST, preferred_element_type=F32)
        square = x * x
        high = square.astype(BF16)
        low = (square - high.astype(F32)).astype(BF16)
        squares = lax.dot_general(ones, high, nt, preferred_element_type=F32) + lax.dot_general(
            ones, low, nt, preferred_element_type=F32
        )
        value = jnp.where(last, squares, own)
        apart = jnp.bitwise_xor(kv_at, k)
        place = lax.rem(apart, half)

        @pl.when(apart < half)
        def _():
            keep_ref[place] = value

        @pl.when(apart >= half)
        def _():
            send_ref[place] = value


def small_sums(pos, blocks, gain, gate_weight, head_local, after):
    count, rows, width = blocks.shape
    shape = (count // 2, 16, rows)
    assert 2 * head_local < 16
    return pl.pallas_call(
        functools.partial(small_body, head_local),
        grid_spec=pltpu.PrefetchScalarGridSpec(
            num_scalar_prefetch=1,
            grid=(1,),
            in_specs=[
                full_spec(blocks.shape),
                pl.BlockSpec((None, 1, width), lambda i, pos_ref: (pos_ref[0], 0, 0)),
                full_spec((gate_weight.shape[1], width)),
                pl.BlockSpec(memory_space=pl.ANY),
            ],
            out_specs=[full_spec(shape), full_spec(shape)],
        ),
        out_shape=[jax.ShapeDtypeStruct(shape, F32)] * 2,
        compiler_params=pltpu.CompilerParams(vmem_limit_bytes=VMEM_LIMIT),
        cost_estimate=pl.CostEstimate(
            flops=100 * count * rows * width, bytes_accessed=2 * count * rows * width, transcendentals=0
        ),
        name="small_sums",
    )(pos, blocks, gain, gate_weight.T, after)


def paths_body(head_local, pos_ref, near_ref, far_ref, bias_ref, parent_ref, stable_ref, decay_ref, _, wmat_ref, cols_ref):
    rows = near_ref.shape[1]
    total = near_ref[...] + far_ref[...]
    row = lax.broadcasted_iota(jnp.int32, (rows, rows), 0)
    lane = lax.broadcasted_iota(jnp.int32, (rows, rows), 1)
    same = row == lane
    parent = parent_ref[...]
    link = ((parent >= 0) & (lane == row // PROP * PROP + parent)).astype(BF16)
    path = (same.astype(F32) + link.astype(F32)).astype(BF16)
    power = link
    reach = 2
    while reach < PROP:
        power = jnp.dot(power, power, preferred_element_type=F32).astype(BF16)
        path = path + jnp.dot(power, path, preferred_element_type=F32).astype(BF16)
        reach *= 2
    path = path.astype(F32)
    on_path = path > 0.5
    scale_row = lax.rsqrt(total[2 * head_local : 2 * head_local + 1] / D + 1e-06)
    scale = jnp.sum(jnp.where(same, scale_row, 0.0), axis=1, keepdims=True)
    for h in range(head_local):
        ingate = total[h : h + 1] * scale_row
        bias = bias_ref[pos_ref[1] * head_local + h]
        raw = total[head_local + h : head_local + h + 1] * scale_row + bias
        logforget = jnp.minimum(raw, 0.0) - jnp.log1p(jnp.exp(-jnp.abs(raw)))
        path_sum = jnp.sum(path * logforget, axis=1, keepdims=True)
        path_row = jnp.sum(jnp.where(same, path_sum, 0.0), axis=0, keepdims=True)
        dlog = jnp.where(on_path, path_sum - path_row + ingate, -jnp.inf)
        carried = path_sum + stable_ref[:, h : h + 1]
        top = jnp.maximum(carried, jnp.max(dlog, axis=1, keepdims=True))
        wmat_ref[h] = jnp.exp(dlog - top) / jnp.sqrt(F32(DQK))
        cols_ref[h, :, 0:1] = scale
        factor = jnp.exp(carried - top)
        cols_ref[h, :, 1:2] = factor
        cols_ref[h, :, 3:4] = factor * decay_ref[:, h : h + 1]
        cols_ref[h, :, 2:3] = jnp.exp(-top)


def path_weights(pos, near, far, bias, parents, stable_rows, decay_rows, head_local, after):
    rows = near.shape[1]
    shapes = [(head_local, rows, rows), (head_local, rows, 4)]
    return pl.pallas_call(
        functools.partial(paths_body, head_local),
        grid_spec=pltpu.PrefetchScalarGridSpec(
            num_scalar_prefetch=1,
            grid=(1,),
            in_specs=[
                full_spec(near.shape),
                full_spec(far.shape),
                pl.BlockSpec(memory_space=pltpu.SMEM),
                full_spec((rows, 1)),
                full_spec(stable_rows.shape),
                full_spec(decay_rows.shape),
                pl.BlockSpec(memory_space=pl.ANY),
            ],
            out_specs=[full_spec(shape) for shape in shapes],
        ),
        out_shape=[jax.ShapeDtypeStruct(shape, F32) for shape in shapes],
        compiler_params=pltpu.CompilerParams(vmem_limit_bytes=VMEM_LIMIT),
        cost_estimate=pl.CostEstimate(
            flops=20 * head_local * rows * rows, bytes_accessed=4 * head_local * rows * rows, transcendentals=0
        ),
        name="path_weights",
    )(pos, near, far, bias, parents.reshape(rows, 1), stable_rows, decay_rows, after)


HEAD_COLS = 2 * DQK + 2 * DV


def full_spec(shape):
    return pl.BlockSpec(shape, lambda i, *_: (0,) * len(shape))


def normed_rows(x_refs, gain_ref, normed_ref):
    at = 0
    for x_ref in x_refs:
        rows = x_ref.shape[0]
        normed_ref[at : at + rows] = (x_ref[...].astype(F32) * gain_ref[...]).astype(BF16)
        at += rows


def project_body(count, pos_ref, *refs):
    x_refs = refs[:count]
    gain_ref, wq_ref, wk_ref, wv_ref, wg_ref, _ = refs[count : count + 6]
    out_refs = refs[count + 6 : -1]
    normed_ref = refs[-1]

    @pl.when(pl.program_id(0) == 0)
    def _():
        normed_rows(x_refs, gain_ref, normed_ref)

    at = 0
    for w_ref in (wq_ref, wk_ref, wv_ref, wg_ref):
        width = w_ref.shape[1]
        product = jnp.dot(normed_ref[...], w_ref[...], preferred_element_type=F32)
        row = 0
        for out_ref in out_refs:
            rows = out_ref.shape[0]
            out_ref[:, at : at + width] = product[row : row + rows].astype(out_ref.dtype)
            row += rows
        at += width


def project(pos, tokens, gain, weights, pieces, dtype, head_local, after, limit):
    width = tokens.shape[2]

    def block(j, offset, rows):
        return pl.BlockSpec(
            (None, rows, width),
            lambda h, pos_ref: (jnp.bitwise_xor(pos_ref[0], j), offset // rows, 0),
        )

    specs = [block(j, offset, rows) for offset, rows, order in pieces for j in order]
    count = len(specs)
    specs.append(pl.BlockSpec((None, 1, width), lambda h, pos_ref: (pos_ref[0], 0, 0)))
    for cols in (DQK, DQK, DV, DV):
        specs.append(pl.BlockSpec((width, cols), lambda h, pos_ref: (0, h)))
    specs.append(pl.BlockSpec(memory_space=pl.ANY))
    outs = [rows * len(order) for _, rows, order in pieces]
    total = sum(outs)
    cols = head_local * HEAD_COLS
    return pl.pallas_call(
        functools.partial(project_body, count),
        grid_spec=pltpu.PrefetchScalarGridSpec(
            num_scalar_prefetch=1,
            grid=(head_local,),
            in_specs=specs,
            out_specs=[pl.BlockSpec((out, HEAD_COLS), lambda h, pos_ref: (0, h)) for out in outs],
            scratch_shapes=[pltpu.VMEM((total, width), BF16)],
        ),
        out_shape=[jax.ShapeDtypeStruct((out, cols), dtype) for out in outs],
        compiler_params=pltpu.CompilerParams(vmem_limit_bytes=limit),
        cost_estimate=pl.CostEstimate(
            flops=2 * total * width * cols,
            bytes_accessed=2 * (total + width) * cols,
            transcendentals=0,
        ),
        name="project_other" if dtype == BF16 else "project_own",
    )(pos, *([tokens] * count), gain, *weights, after)


def fold_body(keep_ref, other_ref, _, out_ref, send_ref, token_ref):
    token_ref[...] = jnp.zeros_like(token_ref)
    rows = out_ref.shape[0]
    out_ref[...] = keep_ref[:rows] + other_ref[:rows].astype(F32)
    send_ref[...] = (keep_ref[rows:] + other_ref[rows:].astype(F32)).astype(BF16)


def fold(keep, other, head_local, after):
    count, cols = keep.shape
    spec = lambda rows: pl.BlockSpec((rows, HEAD_COLS), lambda h: (0, h))
    return pl.pallas_call(
        fold_body,
        grid=(head_local,),
        in_specs=[spec(count), spec(count), pl.BlockSpec(memory_space=pl.ANY)],
        out_specs=[spec(count // 2), spec(count // 2), full_spec(TOKEN)],
        out_shape=[
            jax.ShapeDtypeStruct((count // 2, cols), F32),
            jax.ShapeDtypeStruct((count // 2, cols), BF16),
            jax.ShapeDtypeStruct(TOKEN, F32),
        ],
        compiler_params=pltpu.CompilerParams(vmem_limit_bytes=VMEM_LIMIT),
        cost_estimate=pl.CostEstimate(
            flops=2 * count * cols, bytes_accessed=9 * count * cols, transcendentals=0
        ),
        name="fold",
    )(keep, other, after)


def read_body(head_local, first_seq, own_ref, *refs):
    got_ref, mat_ref, norm_ref, wmat_ref, cols_ref, key_ref, value_ref, weight_ref, gain_ref, _, hid_ref, token_ref = refs
    token_ref[...] = jnp.zeros_like(token_ref)
    rows = own_ref.shape[0]
    seqs = mat_ref.shape[0]
    prop = rows // seqs
    all_seqs = norm_ref.shape[1]
    row_seq = first_seq + lax.broadcasted_iota(jnp.int32, (rows, all_seqs), 0) // prop
    pick = (row_seq == lax.broadcasted_iota(jnp.int32, (rows, all_seqs), 1)).astype(F32)
    lane_seq = lax.broadcasted_iota(jnp.int32, (rows, seqs * DQK), 1) // DQK
    big_seq = lax.broadcasted_iota(jnp.int32, (rows, seqs * DQK), 0) // prop
    big_pick = lane_seq == big_seq
    together = (
        lax.broadcasted_iota(jnp.int32, (rows, rows), 0) // prop
        == lax.broadcasted_iota(jnp.int32, (rows, rows), 1) // prop
    )
    nt = (((1,), (1,)), ((), ()))
    for h in range(head_local):
        base = h * HEAD_COLS

        def total(at, width):
            cols = slice(base + at, base + at + width)
            return own_ref[:, cols] + got_ref[:, cols].astype(F32)

        scale = cols_ref[h, :, 0:1]
        factor = cols_ref[h, :, 1:2]
        floor = cols_ref[h, :, 2:3]
        decayed = cols_ref[h, :, 3:4]
        query = scale * total(0, DQK)
        key = scale * total(DQK, DQK)
        value = scale * total(2 * DQK, DV)
        gate = scale * total(2 * DQK + DV, DV)
        scores = (
            lax.dot_general(query, key, nt, precision=HIGHEST, preferred_element_type=F32)
            * wmat_ref[h]
        )
        numer = jnp.dot(scores, value, precision=HIGHEST, preferred_element_type=F32)
        spread = jnp.where(big_pick, jnp.concatenate([query] * seqs, axis=1), 0.0).astype(BF16)
        mat = mat_ref[:, h].reshape(seqs * DQK, DV).astype(BF16)
        saved = jnp.dot(spread, mat, preferred_element_type=F32)
        prior_key = key_ref[:, h * DQK : (h + 1) * DQK].astype(F32)
        prior = lax.dot_general(query, prior_key, nt, precision=HIGHEST, preferred_element_type=F32)
        prior = jnp.where(together, prior * weight_ref[h : h + 1], 0.0)
        prior_value = value_ref[:, h * DV : (h + 1) * DV].astype(F32)
        added = jnp.dot(prior, prior_value, precision=HIGHEST, preferred_element_type=F32)
        qn = lax.dot_general(query, norm_ref[h], nt, precision=HIGHEST, preferred_element_type=F32)
        denom = jnp.sum(scores, axis=1, keepdims=True) + factor * jnp.sum(
            qn * pick, axis=1, keepdims=True
        )
        read = (numer + decayed * saved + factor * added) / jnp.maximum(jnp.abs(denom), floor)
        normer = lax.rsqrt(jnp.mean(read * read, axis=1, keepdims=True) + 1e-06)
        gain = gain_ref[:, h * DV : (h + 1) * DV]
        hid_ref[:, h * DV : (h + 1) * DV] = (
            read * normer * gain * jax.nn.sigmoid(gate)
        ).astype(BF16)


def tree_read(offset, own, got, mat, norm, wmat, cols, prior, gain, head_local, after):
    rows = own.shape[0]
    seqs = rows // PROP
    keys, values, weights = prior
    return pl.pallas_call(
        functools.partial(read_body, head_local, offset // PROP),
        grid=(1,),
        in_specs=[full_spec(own.shape), full_spec(got.shape)]
        + [
            pl.BlockSpec((seqs,) + mat.shape[1:], lambda i: (offset // rows, 0, 0, 0)),
            full_spec(norm.shape),
            full_spec(wmat.shape),
            pl.BlockSpec((head_local, rows, cols.shape[2]), lambda i: (0, offset // rows, 0)),
            pl.BlockSpec((rows, keys.shape[1]), lambda i: (offset // rows, 0)),
            pl.BlockSpec((rows, values.shape[1]), lambda i: (offset // rows, 0)),
            full_spec(weights.shape),
            full_spec(gain.shape),
            pl.BlockSpec(memory_space=pl.ANY),
        ],
        out_specs=[full_spec((rows, head_local * DV)), full_spec(TOKEN)],
        out_shape=[
            jax.ShapeDtypeStruct((rows, head_local * DV), BF16),
            jax.ShapeDtypeStruct(TOKEN, F32),
        ],
        compiler_params=pltpu.CompilerParams(vmem_limit_bytes=VMEM_MOST),
        cost_estimate=pl.CostEstimate(
            flops=8 * rows * seqs * head_local * DQK * DV,
            bytes_accessed=4 * seqs * head_local * DQK * DV,
            transcendentals=0,
        ),
        name="tree_read",
    )(own, got, mat, norm, wmat, cols, keys, values, weights, gain, after)


def output_body(orders, pos_ref, *refs):
    w_ref = refs[sum(len(order) for order in orders)]
    keep_ref, send_ref = refs[-2:]
    kv_at = pos_ref[0]
    tp_at = pos_ref[1]
    weight = w_ref[...]
    ref_at = 0
    offset = 0
    for order in orders:
        rows = refs[ref_at].shape[0]
        span = slice(offset, offset + rows)
        for distances in order:
            out = jnp.dot(refs[ref_at][...], weight, preferred_element_type=F32)
            ref_at += 1
            for i, j in enumerate(distances):
                piece = out[i * rows : (i + 1) * rows]
                block = jnp.bitwise_xor(kv_at, j)
                apart = jnp.bitwise_xor(lax.div(block, 2), tp_at)
                side = lax.rem(block, 2)
                place = lax.div(apart, 2)
                here = lax.rem(apart, 2) == 0

                @pl.when(here)
                def _():
                    keep_ref[place, side, span] = piece

                @pl.when(jnp.logical_not(here))
                def _():
                    send_ref[place, side, span] = piece

        offset += rows


def output_product(pos, groups, weight, after, tp_size):
    orders = tuple(tuple(distances for distances, _ in group) for group in groups)
    rows = sum(group[0][1].shape[0] for group in groups)
    flat = [value for group in groups for _, value in group]
    shape = (tp_size // 2, 2, rows, weight.shape[1])
    return pl.pallas_call(
        functools.partial(output_body, orders),
        grid_spec=pltpu.PrefetchScalarGridSpec(
            num_scalar_prefetch=1,
            grid=(1,),
            in_specs=[full_spec(value.shape) for value in flat]
            + [full_spec(weight.shape)]
            + [pl.BlockSpec(memory_space=pl.ANY)] * len(after),
            out_specs=[full_spec(shape), full_spec(shape)],
        ),
        out_shape=[jax.ShapeDtypeStruct(shape, F32)] * 2,
        compiler_params=pltpu.CompilerParams(vmem_limit_bytes=VMEM_LIMIT),
        cost_estimate=pl.CostEstimate(
            flops=4 * tp_size * rows * weight.shape[0] * weight.shape[1],
            bytes_accessed=2 * weight.shape[0] * weight.shape[1],
            transcendentals=0,
        ),
        name="output_product",
    )(pos, *flat, weight, *after)


def per_device(
    kv_size,
    tp_size,
    tokens,
    norm_gain,
    query_weight,
    key_weight,
    value_weight,
    outgate_weight,
    gate_weight,
    forget_bias,
    head_gain,
    output_weight,
    state_matrix,
    state_normal,
    state_stable,
    prior_keys,
    prior_values,
    prior_ingate,
    prior_forget,
    accepted,
    parents,
):
    head_local = query_weight.shape[1] // DQK
    width_local = tokens.shape[1]
    seq_local = accepted.shape[0]
    row_local = seq_local * PROP
    unit = row_local // sum(share for share, _ in PLAN)
    bits = [1 << i for i in range(kv_size.bit_length() - 1)]
    chunks = []
    for share, along_z in PLAN:
        steps = bits[1:] + bits[:1] if along_z else bits
        chunks.append((sum(rows for _, rows, _ in chunks), share * unit, steps))
    kv_at = lax.axis_index("kv")
    tp_at = lax.axis_index("tp")
    pos = jnp.stack([kv_at, tp_at]).astype(jnp.int32)

    def swap(value, axis, size, bit):
        return lax.ppermute(value, axis, [(i, i ^ bit) for i in range(size)])

    def across(value, bit):
        return swap(value, "kv", kv_size, bit)

    def near_first(steps):
        order = [0]
        for bit in reversed(steps):
            order = order + [j ^ bit for j in order]
        return order

    weights = (query_weight, key_weight, value_weight, outgate_weight)
    blocks = tokens.reshape(kv_size, row_local, width_local)
    gain_blocks = norm_gain.reshape(kv_size, 1, width_local)

    def project_first(c, after):
        offset, rows, steps = chunks[c]
        order = [j ^ steps[0] for j in near_first(steps[1:])]
        (sent,) = project(
            pos, blocks, gain_blocks, weights, [(offset, rows, order)], BF16, head_local, after,
            VMEM_ALL if c == 0 else VMEM_LIMIT,
        )
        return sent

    count = len(chunks)
    first_sent = project_first(0, pos)
    came = [across(first_sent, chunks[0][2][0])] + [None] * (count - 1)

    token = first_sent
    own = [None] * count
    got = [None] * count
    hidden = [None] * count
    done = {}
    matrices = []

    def run_commit(index, after):
        portion = seq_local // sum(COMMITS)
        factors = commit_factors(prior_keys, prior_values, commit_weights)
        matrix, after = commit_matrix(
            portion * sum(COMMITS[:index]), portion * COMMITS[index], state_matrix, *factors, decay[:, None, :],
            matrices[-1] if matrices else None, after,
        )
        matrices.append(matrix)
        return after

    def prepare(after):
        zero = after[0, 0]
        prior_f32 = prior_keys.astype(F32).reshape(seq_local, PROP, head_local, DQK)
        decay, commit_weights, new_normal, new_stable = commit(
            state_normal, state_stable + zero, prior_f32, prior_ingate, prior_forget + zero, accepted
        )
        return decay, commit_weights, new_normal, new_stable

    gain = head_gain[None, :]

    for event in ORDER:
        kind, c = event[0], int(event[1])
        offset, rows, steps = chunks[c]
        if kind == "g":
            small, away = small_sums(pos, blocks, gain_blocks, gate_weight, head_local, token)
            token = small
            for bit in reversed(bits[1:]):
                total = small + across(away, bit)
                left = total.shape[0] // 2
                small, away = total[:left], total[left:]
            small_far = across(away[0], bits[0])
            small_near = small[0]
        elif kind == "p":
            token = project_first(c, token)
            came[c] = across(token, steps[0])
        elif kind == "o":
            pieces = [(offset, rows, near_first(steps[1:])) for offset, rows, steps in chunks]
            own = project(pos, blocks, gain_blocks, weights, pieces, F32, head_local, token, VMEM_LIMIT)
            own = list(own)
            token = own[0]
        elif kind == "m":
            own[c], send, token = fold(own[c], came[c], head_local, token)
            got[c] = across(send, steps[1])
        elif kind == "s":
            decay, commit_weights, new_normal, new_stable = prepare(token)
            normal_heads = new_normal.transpose(1, 0, 2)
            stable_rows = jnp.repeat(new_stable, PROP, axis=0)
            decay_rows = jnp.repeat(decay, PROP, axis=0)
            prior_rows = (
                prior_keys.reshape(row_local, -1),
                prior_values.reshape(row_local, -1),
                commit_weights.reshape(row_local, head_local).T,
            )
        elif kind == "c":
            token = run_commit(c, token)
        elif kind == "w":
            wmat, cols = path_weights(
                pos, small_near, small_far, forget_bias, parents, stable_rows, decay_rows, head_local, token
            )
            token = cols
        elif kind == "f":
            for bit in steps[2:]:
                own[c], send, token = fold(own[c], got[c], head_local, token)
                got[c] = across(send, bit)
        else:
            span = slice(offset, offset + rows)
            keys, values, weight_row = prior_rows
            hidden[c], token = tree_read(
                offset, own[c], got[c], state_matrix, normal_heads, wmat[:, span, span], cols,
                (keys, values, weight_row[:, span]), gain, head_local, token,
            )
        done[event] = token

    def reduce_out(keep, send):
        got = swap(send, "tp", tp_size, 1)
        total = keep + got
        bit = 2
        while bit < tp_size:
            away = total[1::2].astype(BF16)
            if bit == 2:
                leaving.append(away)
            got = swap(away, "tp", tp_size, bit)
            total = total[::2] + got.astype(F32)
            bit *= 2
        return total[0].astype(BF16)

    def spread(c):
        group = [((0,), hidden[c])]
        if c < count - 1:
            steps = [[bit] for bit in reversed(bits)]
        else:
            steps = [near_first(bits[1:])[1:], [bits[0]]]
        for index, apart in enumerate(steps):
            reach = tuple(j for distances, _ in group for j in distances)
            values = [value for _, value in group]
            have = values[0] if len(values) == 1 else jnp.concatenate(values, axis=0)
            if index > 0:
                last = min(index, len(SPREAD_AFTER[c])) - 1
                have = have + done[SPREAD_AFTER[c][last]][:1, :1].astype(BF16)
            joined[c] = have
            for bit in apart:
                group.append((tuple(j ^ bit for j in reach), across(have, bit)))
        return group

    joined = {}
    leaving = []
    groups = [spread(c) for c in range(count)]
    pieces = []
    while len(matrices) + 1 < len(COMMITS):
        token = run_commit(len(matrices), token)
    for part in OUTPUTS:
        keep, send = output_product(
            pos, [groups[c] for c in part], output_weight, [token] + [joined[c] for c in joined], tp_size
        )
        token = keep
        pieces.append(reduce_out(keep, send))
    run_commit(len(matrices), leaving[-1] if leaving else token)
    new_matrix = matrices[-1]
    layer_out = jnp.concatenate(pieces, axis=1).reshape(2 * row_local, -1)
    return (layer_out, new_matrix, new_normal, new_stable)


def solution(mesh):
    placed = (
        P(None, "kv"),
        P(),
        P("kv", "tp"),
        P("kv", "tp"),
        P("kv", "tp"),
        P("kv", "tp"),
        P("kv", None),
        P(),
        P("tp"),
        P("tp", "kv"),
        P("kv", "tp", None, None),
        P("kv", "tp", None),
        P("kv", "tp"),
        P("kv", None, "tp"),
        P("kv", None, "tp"),
        P("kv", None, "tp"),
        P("kv", None, "tp"),
        P("kv"),
        P("kv", None),
    )
    kv_size = mesh.shape["kv"]
    tp_size = mesh.shape["tp"]
    assert kv_size == 2 * tp_size

    def layered(*args):
        return per_device(kv_size, tp_size, *args)

    return jax.shard_map(
        layered,
        mesh=mesh,
        in_specs=placed,
        out_specs=(P("tp", "kv"), P("kv", "tp", None, None), P("kv", "tp", None), P("kv", "tp")),
        check_vma=False,
    )
```
